32 devices in a mesh: ra: 2 (over core), cb: 4 (over z), dp: 4 (over y, x).
Axes of the slice: x: 2, y: 2, z: 4, core: 2. Of those that a mesh axis runs over, the one named last changes fastest.
Arguments:
- residual_in: bfloat16 [1024, 4096], P('dp', 'cb'), may hold values from -220 to 220, as said below
- gain_in: float32 [4096], P('cb'), may hold values from 0.1 to 1.9
- shift_in: float32 [4096], P('cb'), may hold values from -3 to 3
- up_weight: bfloat16 [4096, 16384], P('cb', 'ra'), may hold values from -0.09375 to 0.09375
- down_weight: bfloat16 [16384, 4096], P('ra', 'cb'), may hold values from -0.046875 to 0.046875
- gain_out: float32 [4096], P('cb'), may hold values from 0.1 to 1.9
- shift_out: float32 [4096], P('cb'), may hold values from -3 to 3
Outputs:
- layer_out: bfloat16 [1024, 4096], P('dp', 'cb')
The draws below stay inside these ranges and needn't reach their ends.
Inputs may be any that keep to these rules, and one draw needn't show every extreme that they name: `residual_in`: real-valued activations.
All inputs are finite; a program needn't handle non-finite values.
Results may differ from the reference program's by a relative error of at most 0.0065.
Values may be sent and summed in bfloat16 or wider, within the bound.
A program may use at most 128 MiB of HBM per device.

```python
import jax
import jax.numpy as jnp
from jax import lax

D = 4096
FF = 16384
TOKENS = 1024


def draw_residual_in(key, part):
    first, second, third = jax.random.split(key, 3)
    column = jnp.arange(D, dtype=jnp.float32) / D
    colscale = 0.5 * jnp.exp(jnp.log(6.0) * column) * jnp.exp(jax.random.uniform(second, (D,), jnp.float32, -0.35, 0.35))
    rowscale = jnp.exp(jax.random.uniform(third, (TOKENS, 1), jnp.float32, 0.0, jnp.log(10.0)))
    noise = jnp.clip(jax.random.normal(first, (TOKENS, D), jnp.float32), -5.0, 5.0)
    values = rowscale * noise * colscale
    return values.astype(jnp.bfloat16)


def steps_of(stream_key, dims, shards, low, high):
    level = 1.0
    for axis_at, parts in shards:
        heights = jax.random.uniform(jax.random.fold_in(jax.random.fold_in(stream_key, 6), axis_at), (parts,), jnp.float32, low / len(shards), high / len(shards))
        level = level * jnp.repeat(jnp.exp(heights), dims[axis_at] // parts).reshape((-1,) + (1,) * (len(dims) - 1 - axis_at))
    return level


def bell_draw(rng, extent, scale, limit, shards=(), kind=jnp.bfloat16):
    level = steps_of(rng, extent, shards, -0.22, 0.18) if shards else 1.0
    values = jax.random.normal(rng, extent, jnp.float32) * scale * level
    return jnp.minimum(jnp.maximum(values, -limit), limit).astype(kind)


def setup_inputs(seed: int = 0) -> dict:
    arg_keys = jax.random.split(jax.random.key(seed), 8)
    residual_in = draw_residual_in(jax.random.fold_in(arg_keys[7], 71), 0)
    gain_in = jnp.clip(1.0 + 0.18 * jax.random.normal(arg_keys[1], (D,), jnp.float32), 0.1, 1.9)
    shift_in = bell_draw(arg_keys[2], (D,), 0.5, 3.0, ((0, 4),), jnp.float32)
    up_weight = bell_draw(arg_keys[3], (D, FF), D ** -0.5, 0.09375, ((0, 4), (1, 2)))
    down_weight = bell_draw(arg_keys[4], (FF, D), FF ** -0.5, 0.046875, ((0, 2), (1, 4)))
    gain_out = jnp.clip(1.0 + 0.18 * jax.random.normal(arg_keys[5], (D,), jnp.float32), 0.1, 1.9)
    shift_out = bell_draw(arg_keys[6], (D,), 0.5, 3.0, ((0, 4),), jnp.float32)
    return {"residual_in": residual_in, "gain_in": gain_in, "shift_in": shift_in, "up_weight": up_weight, "down_weight": down_weight, "gain_out": gain_out, "shift_out": shift_out}


def layer_norm(values, gain, shift):
    mean = lax.optimization_barrier(jnp.mean(values, axis=-1, keepdims=True))
    centred = values - mean
    spread = lax.optimization_barrier(jnp.mean(centred * centred, axis=-1, keepdims=True))
    return centred * jax.lax.rsqrt(spread + 1e-05) * gain + shift

def reference(residual_in, gain_in, shift_in, up_weight, down_weight, gain_out, shift_out):
    normed = layer_norm(residual_in.astype(jnp.float32), gain_in, shift_in).astype(jnp.bfloat16)
    pre = jnp.dot(normed, up_weight, preferred_element_type=jnp.float32)
    hidden = jnp.square(jax.nn.relu(pre)).astype(jnp.bfloat16)
    branch = jnp.dot(hidden, down_weight, preferred_element_type=jnp.float32)
    total = 2.0 ** 0.25 * normed.astype(jnp.float32) + branch
    return layer_norm(total, gain_out, shift_out).astype(jnp.bfloat16)
```

```python
import functools

import jax
import jax.numpy as jnp
from jax import lax
from jax.experimental import pallas as pl
from jax.experimental.pallas import tpu as pltpu
from jax.sharding import PartitionSpec as P

MESH = pl.DeviceIdType.MESH
LANES = 128
STAT_ROWS = 8
CHUNK = 256
WINDOW = 3
LAG = 2
LAG_STEP = 4


def kernel(
    n, n_ra, x_ref, gain_in_ref, shift_in_ref, gain_out_ref, shift_out_ref, up_hbm, down_hbm, out_ref,
    up_v, down_v, sums, from_outer, from_partner, hidden, normed, acc, acc_in, stats_in, stats_out,
    up_sem, down_sem, sums_sent, outer_got, partner_got, hidden_sent, hidden_got,
    stat_sent, stat_got, acc_sent, acc_got,
):
    me = lax.axis_index("cb")
    ra = lax.axis_index("ra")
    chunks, depth, width = up_v.shape
    tokens = x_ref.shape[0]
    half = n // 2
    side = me // half
    level = me * (1 - side) + (n - 1 - me) * side
    inner = lax.rem(me + 1 - 2 * side + n, n)
    outer = lax.rem(me - 1 + 2 * side + n, n)
    is_mid = level == half - 1
    has_outer = level > 0

    def up_copy(c):
        columns = pl.ds(pl.multiple_of(c * width, width), width)
        return pltpu.make_async_copy(up_hbm.at[:, columns], up_v.at[c], up_sem.at[c])

    def down_copy(c):
        rows = pl.ds(pl.multiple_of(c * width, width), width)
        return pltpu.make_async_copy(down_hbm.at[rows, :], down_v.at[c], down_sem.at[c])

    @pl.loop(0, chunks)
    def _(c):
        up_copy(c).start()

    @pl.loop(0, chunks)
    def _(c):
        down_copy(c).start()

    barrier = pltpu.get_barrier_semaphore()
    for k in range(1, n):
        pl.semaphore_signal(barrier, inc=1, device_id={"cb": lax.rem(me + k, n)}, device_id_type=MESH)
    for k in range(1, n_ra):
        pl.semaphore_signal(barrier, inc=1, device_id={"ra": lax.rem(ra + k, n_ra)}, device_id_type=MESH)

    def local_stats(values, stats):
        total = jnp.sum(values, axis=1, keepdims=True)
        centred = values - total * (1.0 / depth)
        squares = jnp.sum(centred * centred, axis=1, keepdims=True)
        lane = lax.broadcasted_iota(jnp.int32, (tokens, LANES), 1)
        tile = jnp.where(lane == 0, total, jnp.where(lane == 1, squares, 0.0))
        stats[me] = tile.T[:STAT_ROWS]

    def stat_copy(stats, which, k, slot):
        return pltpu.make_async_remote_copy(
            src_ref=stats.at[slot], dst_ref=stats.at[slot],
            send_sem=stat_sent.at[which, k], recv_sem=stat_got.at[which, slot],
            device_id={"cb": lax.rem(me + k, n)}, device_id_type=MESH,
        )

    def send_stats(stats, which):
        for k in range(1, n):
            stat_copy(stats, which, k, me).start()

    def merged_stats(stats, which):
        for k in range(1, n):
            stat_copy(stats, which, k, lax.rem(me + k, n)).wait_recv()
        for k in range(1, n):
            stat_copy(stats, which, k, me).wait_send()
        total = stats[0][0:1]
        for j in range(1, n):
            total = total + stats[j][0:1]
        mean = total / (depth * n)
        squares = jnp.zeros_like(mean)
        for j in range(n):
            block = stats[j]
            gap = block[0:1] * (1.0 / depth) - mean
            squares = squares + (block[1:2] + depth * (gap * gap))
        scale = lax.rsqrt(squares / (depth * n) + 1e-05)
        row = lax.broadcasted_iota(jnp.int32, (LANES, tokens), 0)
        tile = jnp.where(row == 0, mean, jnp.where(row == 1, scale, 0.0)).T
        return tile[:, 0:1], tile[:, 1:2]

    values = x_ref[...].astype(jnp.float32)
    local_stats(values, stats_in)
    acc[...] = jnp.zeros_like(acc)
    pl.semaphore_wait(barrier, n - 1 + n_ra - 1)
    send_stats(stats_in, 0)
    mean, scale = merged_stats(stats_in, 0)
    normed[...] = (
        (x_ref[...].astype(jnp.float32) - mean) * scale * gain_in_ref[...] + shift_in_ref[...]
    ).astype(jnp.bfloat16)

    def sum_copy(c, into, got):
        return pltpu.make_async_remote_copy(
            src_ref=sums.at[c], dst_ref=into.at[c], send_sem=sums_sent.at[c], recv_sem=got.at[c],
            device_id={"cb": inner}, device_id_type=MESH,
        )

    def hidden_copy(c):
        return pltpu.make_async_remote_copy(
            src_ref=hidden.at[c], dst_ref=hidden.at[c], send_sem=hidden_sent.at[c],
            recv_sem=hidden_got.at[c], device_id={"cb": outer}, device_id_type=MESH,
        )

    def inward(c):
        up_copy(c).wait()
        part = jnp.dot(normed[...], up_v[c], preferred_element_type=jnp.float32)

        @pl.when(has_outer)
        def _():
            sum_copy(c, from_outer, outer_got).wait_recv()
            sums[c] = (part + from_outer[c].astype(jnp.float32)).astype(jnp.bfloat16)

        @pl.when(level == 0)
        def _():
            sums[c] = part.astype(jnp.bfloat16)

        @pl.when(c >= WINDOW)
        def _():
            sum_copy(c - WINDOW, from_outer, outer_got).wait_send()

        @pl.when(is_mid)
        def _():
            sum_copy(c, from_partner, partner_got).start()

        @pl.when(level < half - 1)
        def _():
            sum_copy(c, from_outer, outer_got).start()

    def outward(c):
        @pl.when(is_mid)
        def _():
            sum_copy(c, from_partner, partner_got).wait_recv()
            full = sums[c].astype(jnp.float32) + from_partner[c].astype(jnp.float32)
            hidden[c] = jnp.square(jnp.maximum(full, 0.0)).astype(jnp.bfloat16)

        @pl.when(level < half - 1)
        def _():
            hidden_copy(c).wait_recv()

        @pl.when(has_outer)
        def _():
            hidden_copy(c).start()

        down_copy(c).wait()
        acc[...] += jnp.dot(hidden[c], down_v[c], preferred_element_type=jnp.float32)

    lag = LAG + LAG_STEP * (half - 1 - level)

    @pl.loop(0, chunks + lag)
    def _(step):
        @pl.when(step < chunks)
        def _():
            inward(step)

        @pl.when(step >= lag)
        def _():
            outward(step - lag)

    def acc_copy(k):
        return pltpu.make_async_remote_copy(
            src_ref=acc, dst_ref=acc_in.at[k - 1], send_sem=acc_sent.at[k - 1], recv_sem=acc_got.at[k - 1],
            device_id={"ra": lax.rem(ra + k, n_ra)}, device_id_type=MESH,
        )

    for k in range(1, n_ra):
        acc_copy(k).start()

    @pl.loop(max(chunks - WINDOW, 0), chunks)
    def _(c):
        sum_copy(c, from_outer, outer_got).wait_send()

    @pl.when(has_outer)
    def _():
        @pl.loop(0, chunks)
        def _(c):
            hidden_copy(c).wait_send()

    for k in range(1, n_ra):
        acc_copy(k).wait()
    branch = acc[...]
    for k in range(1, n_ra):
        branch = branch + acc_in[k - 1]
    total = 2.0**0.25 * normed[...].astype(jnp.float32) + branch
    acc[...] = total
    local_stats(total, stats_out)
    send_stats(stats_out, 1)
    mean, scale = merged_stats(stats_out, 1)
    out_ref[...] = ((acc[...] - mean) * scale * gain_out_ref[...] + shift_out_ref[...]).astype(jnp.bfloat16)


def solution(mesh):
    n, n_ra = mesh.shape["cb"], mesh.shape["ra"]

    def per_device(residual_in, gain_in, shift_in, up_weight, down_weight, gain_out, shift_out):
        tokens, depth = residual_in.shape
        units = up_weight.shape[1]
        width = CHUNK if units % CHUNK == 0 else units
        chunks = units // width
        vmem = pl.BlockSpec(memory_space=pltpu.VMEM)
        hbm = pl.BlockSpec(memory_space=pl.ANY)
        block = (chunks, tokens, width)
        return pl.pallas_call(
            functools.partial(kernel, n, n_ra),
            out_shape=jax.ShapeDtypeStruct((tokens, depth), jnp.bfloat16),
            in_specs=[vmem] * 5 + [hbm] * 2,
            out_specs=vmem,
            scratch_shapes=[
                pltpu.VMEM((chunks, depth, width), jnp.bfloat16),
                pltpu.VMEM((chunks, width, depth), jnp.bfloat16),
                pltpu.VMEM(block, jnp.bfloat16),
                pltpu.VMEM(block, jnp.bfloat16),
                pltpu.VMEM(block, jnp.bfloat16),
                pltpu.VMEM(block, jnp.bfloat16),
                pltpu.VMEM((tokens, depth), jnp.bfloat16),
                pltpu.VMEM((tokens, depth), jnp.float32),
                pltpu.VMEM((n_ra - 1, tokens, depth), jnp.float32),
                pltpu.VMEM((n, STAT_ROWS, tokens), jnp.float32),
                pltpu.VMEM((n, STAT_ROWS, tokens), jnp.float32),
            ]
            + [pltpu.SemaphoreType.DMA((chunks,))] * 7
            + [pltpu.SemaphoreType.DMA((2, n))] * 2
            + [pltpu.SemaphoreType.DMA((n_ra - 1,))] * 2,
            compiler_params=pltpu.CompilerParams(
                collective_id=0, has_side_effects=True, vmem_limit_bytes=64 * 1000 * 1024
            ),
        )(
            residual_in, gain_in.reshape(1, depth), shift_in.reshape(1, depth),
            gain_out.reshape(1, depth), shift_out.reshape(1, depth), up_weight, down_weight,
        )

    in_specs = (P("dp", "cb"), P("cb"), P("cb"), P("cb", "ra"), P("ra", "cb"), P("cb"), P("cb"))
    return jax.shard_map(
        per_device, mesh=mesh, in_specs=in_specs, out_specs=P("dp", "cb"), check_vma=False
    )
```

```python
import functools

import jax
import jax.numpy as jnp
from jax import lax
from jax.experimental import pallas as pl
from jax.experimental.pallas import tpu as pltpu
from jax.sharding import PartitionSpec as P

MESH = pl.DeviceIdType.MESH
LANES = 128
STAT_ROWS = 8
CHUNK = 256
WINDOW = 4
LAG = 3
AHEAD = 8
SPLIT = 2
LAG_STEP = 7


def kernel(
    n, n_ra, x_ref, gain_in_ref, shift_in_ref, gain_out_ref, shift_out_ref, up_hbm, down_hbm, out_ref,
    up_v, down_v, tile_v, sums, from_outer, from_partner, hidden, normed, acc, acc_in, stats_in, stats_out,
    up_sem, down_sem, sums_sent, outer_got, partner_got, hidden_sent, hidden_got,
    stat_sent, stat_got, acc_sent, acc_got,
):
    me = lax.axis_index("cb")
    ra = lax.axis_index("ra")
    chunks, depth, width = up_v.shape
    tokens = x_ref.shape[0]
    steps, rows = sums.shape[0], sums.shape[1]
    split = steps // chunks
    half = n // 2
    ahead = min(AHEAD, chunks)
    side = me // half
    level = me * (1 - side) + (n - 1 - me) * side
    inner = lax.rem(me + 1 - 2 * side + n, n)
    outer = lax.rem(me - 1 + 2 * side + n, n)
    is_mid = level == half - 1
    has_outer = level > 0

    def up_copy(c):
        columns = pl.ds(pl.multiple_of(c * width, width), width)
        return pltpu.make_async_copy(up_hbm.at[:, columns], up_v.at[c], up_sem.at[c])

    def down_copy(c):
        rows = pl.ds(pl.multiple_of(c * width, width), width)
        return pltpu.make_async_copy(down_hbm.at[rows, :], down_v.at[c], down_sem.at[c])

    barrier = pltpu.get_barrier_semaphore()
    for k in range(1, n):
        pl.semaphore_signal(barrier, inc=1, device_id={"cb": lax.rem(me + k, n)}, device_id_type=MESH)
    for k in range(1, n_ra):
        pl.semaphore_signal(barrier, inc=1, device_id={"ra": lax.rem(ra + k, n_ra)}, device_id_type=MESH)

    for c in range(ahead):
        up_copy(c).start()

    def row_stats(values):
        total = jnp.sum(values, axis=1, keepdims=True)
        centred = values - total * (1.0 / depth)
        squares = jnp.sum(centred * centred, axis=1, keepdims=True)
        lane = lax.broadcasted_iota(jnp.int32, (values.shape[0], LANES), 1)
        return jnp.where(lane == 0, total, jnp.where(lane == 1, squares, 0.0))

    def stat_copy(stats, which, k, slot):
        return pltpu.make_async_remote_copy(
            src_ref=stats.at[slot], dst_ref=stats.at[slot],
            send_sem=stat_sent.at[which, k], recv_sem=stat_got.at[which, slot],
            device_id={"cb": lax.rem(me + k, n)}, device_id_type=MESH,
        )

    def send_stats(stats, which):
        for k in range(1, n):
            stat_copy(stats, which, k, me).start()

    def merged_stats(stats, which):
        for k in range(1, n):
            stat_copy(stats, which, k, lax.rem(me + k, n)).wait_recv()
        for k in range(1, n):
            stat_copy(stats, which, k, me).wait_send()
        total = stats[0][0:1]
        for j in range(1, n):
            total = total + stats[j][0:1]
        mean = total / (depth * n)
        squares = jnp.zeros_like(mean)
        for j in range(n):
            block = stats[j]
            gap = block[0:1] * (1.0 / depth) - mean
            squares = squares + (block[1:2] + depth * (gap * gap))
        scale = lax.rsqrt(squares / (depth * n) + 1e-05)
        row = lax.broadcasted_iota(jnp.int32, (LANES, tokens), 0)
        tile = jnp.where(row == 0, mean, jnp.where(row == 1, scale, 0.0)).T
        return tile[:, 0:1], tile[:, 1:2]

    values = x_ref[...].astype(jnp.float32)
    stats_in[me] = row_stats(values).T[:STAT_ROWS]
    acc[...] = jnp.zeros_like(acc)
    pl.semaphore_wait(barrier, n - 1 + n_ra - 1)
    send_stats(stats_in, 0)
    for c in range(ahead):
        down_copy(c).start()
    mean, scale = merged_stats(stats_in, 0)
    normed[...] = (
        (x_ref[...].astype(jnp.float32) - mean) * scale * gain_in_ref[...] + shift_in_ref[...]
    ).astype(jnp.bfloat16)

    def sum_copy(c, into, got):
        return pltpu.make_async_remote_copy(
            src_ref=sums.at[c], dst_ref=into.at[c], send_sem=sums_sent.at[c], recv_sem=got.at[c],
            device_id={"cb": inner}, device_id_type=MESH,
        )

    def hidden_copy(c):
        return pltpu.make_async_remote_copy(
            src_ref=hidden.at[c], dst_ref=hidden.at[c], send_sem=hidden_sent.at[c],
            recv_sem=hidden_got.at[c], device_id={"cb": outer}, device_id_type=MESH,
        )

    def block_of(r):
        return pl.ds(pl.multiple_of(r * rows, rows), rows)

    def acc_copy(k, r):
        return pltpu.make_async_remote_copy(
            src_ref=acc.at[block_of(r)], dst_ref=acc_in.at[k - 1, block_of(r)],
            send_sem=acc_sent.at[k - 1, r], recv_sem=acc_got.at[k - 1, r],
            device_id={"ra": lax.rem(ra + k, n_ra)}, device_id_type=MESH,
        )

    def inward(c):
        unit, r = c // split, lax.rem(c, split)

        @pl.when(r == 0)
        def _():
            up_copy(unit).wait()

            @pl.when(unit + ahead < chunks)
            def _():
                up_copy(unit + ahead).start()
                down_copy(unit + ahead).start()

        part = jnp.dot(normed[block_of(r)], up_v[unit], preferred_element_type=jnp.float32)

        @pl.when(has_outer)
        def _():
            sum_copy(c, from_outer, outer_got).wait_recv()
            sums[c] = (part + from_outer[c].astype(jnp.float32)).astype(jnp.bfloat16)

        @pl.when(level == 0)
        def _():
            sums[c] = part.astype(jnp.bfloat16)

        @pl.when(c >= WINDOW)
        def _():
            sum_copy(c - WINDOW, from_outer, outer_got).wait_send()

        @pl.when(is_mid)
        def _():
            sum_copy(c, from_partner, partner_got).start()

        @pl.when(level < half - 1)
        def _():
            sum_copy(c, from_outer, outer_got).start()

    def outward(c):
        @pl.when(is_mid)
        def _():
            sum_copy(c, from_partner, partner_got).wait_recv()
            full = sums[c].astype(jnp.float32) + from_partner[c].astype(jnp.float32)
            hidden[c] = jnp.square(jnp.maximum(full, 0.0)).astype(jnp.bfloat16)

        @pl.when(level < half - 1)
        def _():
            hidden_copy(c).wait_recv()

        @pl.when(has_outer)
        def _():
            hidden_copy(c).start()

        unit, r = c // split, lax.rem(c, split)

        @pl.when(r == 0)
        def _():
            down_copy(unit).wait()

        acc[block_of(r)] += jnp.dot(hidden[c], down_v[unit], preferred_element_type=jnp.float32)

        @pl.when(unit == chunks - 1)
        def _():
            for k in range(1, n_ra):
                acc_copy(k, r).start()

    lag = LAG + LAG_STEP * (half - 1 - level)

    @pl.loop(0, steps + lag)
    def _(step):
        @pl.when(step < steps)
        def _():
            inward(step)

        @pl.when(step >= lag)
        def _():
            outward(step - lag)

    @pl.loop(max(steps - WINDOW, 0), steps)
    def _(c):
        sum_copy(c, from_outer, outer_got).wait_send()

    @pl.when(has_outer)
    def _():
        @pl.loop(0, steps)
        def _(c):
            hidden_copy(c).wait_send()

    for r in range(split):
        block = pl.ds(r * rows, rows)
        for k in range(1, n_ra):
            acc_copy(k, r).wait()
        branch = acc[block]
        for k in range(1, n_ra):
            branch = branch + acc_in[k - 1, block]
        total = 2.0**0.25 * normed[block].astype(jnp.float32) + branch
        acc[block] = total
        tile_v[block] = row_stats(total)
    stats_out[me] = tile_v[...].T[:STAT_ROWS]
    send_stats(stats_out, 1)
    mean, scale = merged_stats(stats_out, 1)
    out_ref[...] = ((acc[...] - mean) * scale * gain_out_ref[...] + shift_out_ref[...]).astype(jnp.bfloat16)


def solution(mesh):
    n, n_ra = mesh.shape["cb"], mesh.shape["ra"]

    def per_device(residual_in, gain_in, shift_in, up_weight, down_weight, gain_out, shift_out):
        tokens, depth = residual_in.shape
        units = up_weight.shape[1]
        width = CHUNK if units % CHUNK == 0 else units
        chunks = units // width
        vmem = pl.BlockSpec(memory_space=pltpu.VMEM)
        hbm = pl.BlockSpec(memory_space=pl.ANY)
        split = SPLIT if tokens % (SPLIT * LANES // 2) == 0 else 1
        block = (chunks * split, tokens // split, width)
        return pl.pallas_call(
            functools.partial(kernel, n, n_ra),
            out_shape=jax.ShapeDtypeStruct((tokens, depth), jnp.bfloat16),
            in_specs=[vmem] * 5 + [hbm] * 2,
            out_specs=vmem,
            scratch_shapes=[
                pltpu.VMEM((chunks, depth, width), jnp.bfloat16),
                pltpu.VMEM((chunks, width, depth), jnp.bfloat16),
                pltpu.VMEM((tokens, LANES), jnp.float32),
                pltpu.VMEM(block, jnp.bfloat16),
                pltpu.VMEM(block, jnp.bfloat16),
                pltpu.VMEM(block, jnp.bfloat16),
                pltpu.VMEM(block, jnp.bfloat16),
                pltpu.VMEM((tokens, depth), jnp.bfloat16),
                pltpu.VMEM((tokens, depth), jnp.float32),
                pltpu.VMEM((n_ra - 1, tokens, depth), jnp.float32),
                pltpu.VMEM((n, STAT_ROWS, tokens), jnp.float32),
                pltpu.VMEM((n, STAT_ROWS, tokens), jnp.float32),
            ]
            + [pltpu.SemaphoreType.DMA((chunks,))] * 2
            + [pltpu.SemaphoreType.DMA((chunks * split,))] * 5
            + [pltpu.SemaphoreType.DMA((2, n))] * 2
            + [pltpu.SemaphoreType.DMA((n_ra - 1, split))] * 2,
            compiler_params=pltpu.CompilerParams(
                collective_id=0, has_side_effects=True, vmem_limit_bytes=64 * 1000 * 1024
            ),
        )(
            residual_in, gain_in.reshape(1, depth), shift_in.reshape(1, depth),
            gain_out.reshape(1, depth), shift_out.reshape(1, depth), up_weight, down_weight,
        )

    in_specs = (P("dp", "cb"), P("cb"), P("cb"), P("cb", "ra"), P("ra", "cb"), P("cb"), P("cb"))
    return jax.shard_map(
        per_device, mesh=mesh, in_specs=in_specs, out_specs=P("dp", "cb"), check_vma=False
    )
```
